32 devices in a mesh: rep: 4 (over z), fs: 2 (over y), tp: 4 (over x, core).
Axes of the slice: x: 2, y: 2, z: 4, core: 2. Of those that a mesh axis runs over, the one named last changes fastest.
Arguments:
- inputs: bfloat16 [512, 4096], P('rep'), may hold values from -6 to 6
- cotangent: bfloat16 [512, 4096], P('rep'), may hold values from -6 to 6
- w_gate: bfloat16 [4096, 11264], P(None, ('fs', 'tp')), may hold values from -0.09375 to 0.09375
- w_upward: bfloat16 [4096, 11264], P(None, ('fs', 'tp')), may hold values from -0.09375 to 0.09375
- w_down: bfloat16 [11264, 4096], P(('fs', 'tp')), may hold values from -0.0546875 to 0.0546875
Outputs:
- grad_input: bfloat16 [512, 4096], P('rep')
- grad_gate: float32 [4096, 11264], P('rep', ('fs', 'tp'))
- grad_upward: float32 [4096, 11264], P('rep', ('fs', 'tp'))
- grad_down: float32 [11264, 4096], P(('fs', 'tp'), 'rep')
The draws below stay inside these ranges and needn't reach their ends.
All inputs are finite; a program needn't handle non-finite values.
Results may differ from the reference program's by a relative error of at most 0.0049.
Values may be sent and summed in bfloat16 or wider, within the bound.
A program may use at most 128 MiB of HBM per device.

```python
import jax
import jax.numpy as jnp

D = 4096
FF = 11264
TOKENS = 512


def spiked(result, rng, source, target, parts, factor):
    owner, partner = [(jnp.arange(result.shape[position]) // (result.shape[position] // parts)).reshape([-1 if axis == position else 1 for axis in range(result.ndim)]) for position in (source, target)]
    chosen = jax.random.permutation(rng, parts)[partner]
    strong = (owner == chosen) | (owner == (partner + parts // 2) % parts)
    return jnp.where(strong, factor * result, result)


def shard_levels(stream_key, extent, split, smallest, largest):
    loudness, own = 1.0, jax.random.fold_in(stream_key, 6)
    for position, shards_of in split:
        draws = jnp.exp(jax.random.uniform(jax.random.fold_in(own, position), (shards_of,), jnp.float32, smallest / len(split), largest / len(split)))
        loudness = loudness * jnp.repeat(draws, extent[position] // shards_of).reshape([-1 if axis == position else 1 for axis in range(len(extent))])
    return loudness


def centred(rng, shape, spread, reach, pieces=(), dtype=jnp.bfloat16):
    values = jax.random.normal(rng, shape, jnp.float32) * spread
    if len(pieces) > 0:
        values = shard_levels(rng, shape, pieces, -0.22, 0.18) * values
    return jnp.clip(values, min=-reach, max=reach).astype(dtype)


def bell_draw_with(own_key, dims, scale, limit, split, heavy, dtype=jnp.bfloat16):
    drawn = scale * jax.random.normal(own_key, dims, jnp.float32)
    if split:
        drawn = drawn * shard_levels(own_key, dims, split, -0.22, 0.18)
    return jnp.clip(spiked(drawn, jax.random.fold_in(own_key, 3), *heavy), -limit, limit).astype(dtype)


def setup_inputs(seed: int = 0) -> dict:
    keys = jax.random.split(jax.random.key(seed), 6)
    inputs = centred(keys[0], (TOKENS, D), 1.0, 6.0, ((0, 4),))
    cotangent = bell_draw_with(keys[1], (TOKENS, D), 1.0, 6.0, ((0, 4),), (0, 1, 4, 2.0))
    w_gate = centred(keys[2], (D, FF), D ** -0.5, 0.09375, ((1, 8),))
    w_upward = centred(keys[3], (D, FF), D ** -0.5, 0.09375, ((1, 8),))
    w_down = centred(keys[4], (FF, D), FF ** -0.5, 0.0546875, ((0, 8),))
    return {"inputs": inputs, "cotangent": cotangent, "w_gate": w_gate, "w_upward": w_upward, "w_down": w_down}


def reference(inputs, cotangent, w_gate, w_upward, w_down):
    gate_pre = jnp.dot(inputs, w_gate, preferred_element_type=jnp.float32)
    up_pre = jnp.dot(inputs, w_upward, preferred_element_type=jnp.float32)
    sigmoid_gate = jax.nn.sigmoid(gate_pre)
    activated = gate_pre * sigmoid_gate
    hidden = (activated * up_pre).astype(jnp.bfloat16)
    hidden_grad = jnp.dot(cotangent, w_down.T, preferred_element_type=jnp.float32)
    gate_delta = (hidden_grad * up_pre * sigmoid_gate * (1.0 + gate_pre * (1.0 - sigmoid_gate))).astype(jnp.bfloat16)
    up_delta = (hidden_grad * activated).astype(jnp.bfloat16)
    grad_input = (jnp.dot(gate_delta, w_gate.T, preferred_element_type=jnp.float32)
                  + jnp.dot(up_delta, w_upward.T, preferred_element_type=jnp.float32)).astype(jnp.bfloat16)
    grad_gate = jnp.dot(inputs.T, gate_delta, preferred_element_type=jnp.float32)
    grad_upward = jnp.dot(inputs.T, up_delta, preferred_element_type=jnp.float32)
    grad_down = jnp.dot(hidden.T, cotangent, preferred_element_type=jnp.float32)
    return (grad_input, grad_gate, grad_upward, grad_down)
```

```python
import functools

import jax
import jax.numpy as jnp
from jax import lax
from jax.experimental import pallas as pl
from jax.experimental.pallas import tpu as pltpu
from jax.sharding import PartitionSpec as P

PLANE = ("fs", "tp")
MESH = pl.DeviceIdType.MESH


def contract_rows(left, right):
    return lax.dot_general(
        left, right, (((0,), (0,)), ((), ())), preferred_element_type=jnp.float32
    )


def contract_cols(left, right):
    return lax.dot_general(
        left, right, (((1,), (1,)), ((), ())), preferred_element_type=jnp.float32
    )


def greet(neighbours):
    barrier = pltpu.get_barrier_semaphore()
    for device in neighbours:
        pl.semaphore_signal(barrier, inc=1, device_id=device, device_id_type=MESH)
    pl.semaphore_wait(barrier, len(neighbours))


def gather_kernel(reps, x_ref, c_ref, all_x, all_c, send, recv, own_sem):
    z, y, t = lax.axis_index("rep"), lax.axis_index("fs"), lax.axis_index("tp")
    x, core = t // 2, t % 2
    half = (x + y) % 2
    mine = 2 * half + core
    across = 2 * (1 - half) + core
    up, down = (z + 1) % reps, (z + reps - 1) % reps
    to_up, to_down = (up, y, t), (down, y, t)
    x_near = (z, y, 2 * (x + 1 - 2 * (x % 2)) + core)
    y_near = (z, y + 1 - 2 * (y % 2), t)
    other = (z, y, 2 * x + 1 - core)
    greet((to_up, to_down, x_near, y_near, other))

    started = []

    def put(kind, step, src, dst, device):
        copy = pltpu.make_async_remote_copy(
            src_ref=src, dst_ref=dst, send_sem=send.at[kind, step],
            recv_sem=recv.at[kind, step], device_id=device, device_id_type=MESH,
        )
        copy.start()
        started.append(copy)
        return copy

    ring = [
        put(0, 0, x_ref.at[mine], all_x.at[z, mine], to_up),
        put(1, 0, c_ref.at[mine], all_c.at[z, mine], to_down),
    ]
    keep = [
        pltpu.make_async_copy(x_ref, all_x.at[z], own_sem.at[0]),
        pltpu.make_async_copy(c_ref, all_c.at[z], own_sem.at[1]),
    ]
    for copy in keep:
        copy.start()

    last = []

    def relay(sides, step, bx, bc):
        sides[0].wait_recv()
        last.append(put(6, step, all_x.at[bx, across], all_x.at[bx, across], other))
        sides[1].wait_recv()
        last.append(put(7, step, all_c.at[bc, across], all_c.at[bc, across], other))

    before = None
    for step in range(reps - 1):
        bx, bc = (z + reps - 1 - step) % reps, (z + 1 + step) % reps
        got_x, got_c = all_x.at[bx, mine], all_c.at[bc, mine]
        following = []
        ring[0].wait_recv()
        if step < reps - 2:
            following.append(put(0, step + 1, got_x, got_x, to_up))
        side_x = put(2, step, got_x, got_x, x_near)
        last.append(put(4, step, got_x, got_x, other))
        ring[1].wait_recv()
        if step < reps - 2:
            following.append(put(1, step + 1, got_c, got_c, to_down))
        side_c = put(3, step, got_c, got_c, y_near)
        last.append(put(5, step, got_c, got_c, other))
        if before is not None:
            relay(*before)
        before = ((side_x, side_c), step, bx, bc)
        ring = following
    relay(*before)
    for copy in last:
        copy.wait_recv()
    for copy in started:
        copy.wait_send()
    for copy in keep:
        copy.wait()


def gather(reps, inputs, cotangent):
    rows, width = inputs.shape
    quarter = (4, rows // 4, width)
    whole = jax.ShapeDtypeStruct((reps,) + quarter, inputs.dtype)
    vmem = pl.BlockSpec(memory_space=pltpu.VMEM)
    pair = pl.pallas_call(
        functools.partial(gather_kernel, reps),
        out_shape=(whole, whole),
        in_specs=[vmem, vmem],
        out_specs=(vmem, vmem),
        scratch_shapes=[
            pltpu.SemaphoreType.DMA((8, reps - 1)),
            pltpu.SemaphoreType.DMA((8, reps - 1)),
            pltpu.SemaphoreType.DMA((2,)),
        ],
        compiler_params=pltpu.CompilerParams(
            collective_id=0, has_side_effects=True, vmem_limit_bytes=60 * 2**20
        ),
        name="token_gather",
    )(inputs.reshape(quarter), cotangent.reshape(quarter))
    return [a.reshape(reps * rows, width) for a in pair]


def reduce_kernel(chips, across, terms, out, got, sums, landed, send, recv):
    z, y, t = lax.axis_index("rep"), lax.axis_index("fs"), lax.axis_index("tp")
    core = t % 2
    chip = y * across + t // 2
    other = (z, y, t + 1 - 2 * core)

    def peer(ahead):
        there = (chip + ahead) % chips
        return there, (z, there // across, 2 * (there % across) + core)

    greet([other] + [peer(ahead)[1] for ahead in range(1, chips)])

    def put(kind, slot, src, dst, device):
        copy = pltpu.make_async_remote_copy(
            src_ref=src, dst_ref=dst, send_sem=send.at[kind, slot],
            recv_sem=recv.at[kind, slot], device_id=device, device_id_type=MESH,
        )
        copy.start()
        return copy

    swaps = [put(0, j, terms.at[j, 1 - core], got.at[j], other) for j in range(chips)]
    for j in range(chips):
        swaps[j].wait_recv()
        pair = terms[j, core].astype(jnp.float32) + got[j].astype(jnp.float32)
        sums[j] = pair.astype(sums.dtype)
    spread = []
    for ahead in range(1, chips):
        there, device = peer(ahead)
        spread.append(put(1, ahead, sums.at[there], landed.at[ahead], device))
    total = terms[chip, core].astype(jnp.float32) + got[chip].astype(jnp.float32)
    for ahead in range(1, chips):
        spread[ahead - 1].wait_recv()
        total = total + landed[ahead].astype(jnp.float32)
    out[chip, core] = total.astype(out.dtype)
    done = out.at[chip, core]
    share = [put(2, ahead, done, done, peer(ahead)[1]) for ahead in range(1, chips)]
    relays = [put(3, 0, done, done, other)]
    for ahead in range(1, chips):
        share[ahead - 1].wait_recv()
        source = out.at[(chip + chips - ahead) % chips, core]
        relays.append(put(3, ahead, source, source, other))
    for copy in relays:
        copy.wait_recv()
    for copy in swaps + spread + share + relays:
        copy.wait_send()


def plane_sum(chips, across, terms):
    rows, width = terms.shape
    piece = (rows // (2 * chips), width)
    vmem = pl.BlockSpec(memory_space=pltpu.VMEM)
    total = pl.pallas_call(
        functools.partial(reduce_kernel, chips, across),
        out_shape=jax.ShapeDtypeStruct((chips, 2) + piece, terms.dtype),
        in_specs=[vmem],
        out_specs=vmem,
        scratch_shapes=[
            pltpu.VMEM((chips,) + piece, terms.dtype),
            pltpu.VMEM((chips,) + piece, terms.dtype),
            pltpu.VMEM((chips,) + piece, terms.dtype),
            pltpu.SemaphoreType.DMA((4, chips)),
            pltpu.SemaphoreType.DMA((4, chips)),
        ],
        compiler_params=pltpu.CompilerParams(
            collective_id=1, has_side_effects=True, vmem_limit_bytes=48 * 2**20
        ),
        name="plane_sum",
    )(terms.reshape((chips, 2) + piece))
    return total.reshape(rows, width)


def chunks_of(total, width):
    return [(at, min(width, total - at)) for at in range(0, total, width)]


def fused_kernel(
    reps, chips, across, x_hbm, c_hbm, wg_hbm, wu_hbm, wd_hbm,
    out, hid, gd, ud, xc, cc,
    all_x, all_c, wg, wu, wd, gpre, upre, terms, got, sums, landed,
    send, recv, sum_send, sum_recv, local_sem, weight_sem,
):
    z, y, t = lax.axis_index("rep"), lax.axis_index("fs"), lax.axis_index("tp")
    x, core = t // 2, t % 2
    rows, width = all_x.shape[1:]
    hidden = wg.shape[1]
    quarter = rows // 4
    cols = width // reps
    half = (x + y) % 2
    mine = 2 * half + core
    over = 2 * (1 - half) + core
    chip = y * across + x
    x_near = (z, y, 2 * (x + 1 - 2 * (x % 2)) + core)
    y_near = (z, y + 1 - 2 * (y % 2), t)
    other = (z, y, 2 * x + 1 - core)
    pieces = chunks_of(hidden, 512)

    def peer(ahead):
        there = (chip + ahead) % chips
        return there, (z, there // across, 2 * (there % across) + core)

    def rows_of(part):
        return pl.ds(pl.multiple_of(part * quarter, quarter), quarter)

    local = [
        pltpu.make_async_copy(x_hbm, all_x.at[z], local_sem.at[0]),
        pltpu.make_async_copy(c_hbm, all_c.at[z], local_sem.at[1]),
    ]
    for copy in local:
        copy.start()
    weights = []
    for at, size in pieces:
        n = len(weights)
        span = pl.ds(at, size)
        weights.append([
            pltpu.make_async_copy(wg_hbm.at[:, span], wg.at[:, span], weight_sem.at[n, 0]),
            pltpu.make_async_copy(wu_hbm.at[:, span], wu.at[:, span], weight_sem.at[n, 1]),
            pltpu.make_async_copy(wd_hbm.at[span], wd.at[span], weight_sem.at[n, 2]),
        ])
        for copy in weights[-1]:
            copy.start()

    greet(
        [((z + 1) % reps, y, t), ((z + reps - 1) % reps, y, t), other]
        + [peer(ahead)[1] for ahead in range(1, chips)]
    )

    def make(kind, block, src, dst, device, sender=None):
        return pltpu.make_async_remote_copy(
            src_ref=src, dst_ref=dst, send_sem=send.at[kind if sender is None else sender, block],
            recv_sem=recv.at[kind, block], device_id=device, device_id_type=MESH,
        )

    started = []

    def put(condition, copy):
        if condition is None:
            copy.start()
        else:
            pl.when(condition)(copy.start)
        started.append((condition, copy))
        return copy

    own = rows_of(mine)
    for kind, src, dst in ((0, x_hbm, all_x), (1, c_hbm, all_c)):
        put(z < reps - 1, make(kind, z, src.at[own], dst.at[z, own], (jnp.minimum(z + 1, reps - 1), y, t)))
        put(z > 0, make(kind, z, src.at[own], dst.at[z, own], (jnp.maximum(z - 1, 0), y, t), 8 + kind))

    def sides(step):
        low, high = z - 1 - step, z + 1 + step
        return (
            (low >= 0, jnp.maximum(low, 0), jnp.minimum(z + 1, reps - 1), (low >= 0) & (z < reps - 1)),
            (high < reps, jnp.minimum(high, reps - 1), jnp.maximum(z - 1, 0), (high < reps) & (z > 0)),
        )

    def guarded(condition, action):
        pl.when(condition)(action)

    def hop(array, step):
        buffer = (all_x, all_c)[array]
        near = (x_near, y_near)[array]
        for valid, block, onward, passes in sides(step):
            piece = buffer.at[block, own]
            arrived = make(array, block, piece, piece, other)
            guarded(valid, arrived.wait_recv)
            put(passes, make(array, block, piece, piece, (onward, y, t)))
            put(valid, make(2 + array, block, piece, piece, near))
            put(valid, make(4 + array, block, piece, piece, other))

    def relay(array, step):
        buffer = (all_x, all_c)[array]
        far = rows_of(over)
        for valid, block, _, _ in sides(step):
            piece = buffer.at[block, far]
            arrived = make(2 + array, block, piece, piece, other)
            guarded(valid, arrived.wait_recv)
            put(valid, make(6 + array, block, piece, piece, other))

    def complete(array, block):
        buffer = (all_x, all_c)[array]
        for kind in (4, 6):
            piece = buffer.at[block, own]
            make(kind + array, block, piece, piece, other).wait_recv()

    def pre(block, at, size):
        span = pl.ds(at, size)
        tokens = all_x[block]
        gpre[:, span] = jnp.dot(tokens, wg[:, span], preferred_element_type=jnp.float32)
        upre[:, span] = jnp.dot(tokens, wu[:, span], preferred_element_type=jnp.float32)

    def deltas(block, at, size):
        span = pl.ds(at, size)
        grad = contract_cols(all_c[block], wd[span, :])
        gate, up = gpre[:, span], upre[:, span]
        sig = jax.nn.sigmoid(gate)
        act = gate * sig
        hid[block, :, span] = (act * up).astype(hid.dtype)
        gd[block, :, span] = (grad * up * sig * (1.0 + gate * (1.0 - sig))).astype(gd.dtype)
        ud[block, :, span] = (grad * act).astype(ud.dtype)

    def keep_cols(array, block):
        span = pl.ds(pl.multiple_of(z * cols, cols), cols)
        source, target = ((all_x, xc), (all_c, cc))[array]
        target[block] = source[block, :, span]

    for copy in local:
        copy.wait()
    for n, (at, size) in enumerate(pieces):
        weights[n][0].wait()
        weights[n][1].wait()
        pre(z, at, size)
        weights[n][2].wait()
        deltas(z, at, size)
        if n == 1:
            hop(0, 0)

    part = width // 4
    for n in range(4):
        span = pl.ds(n * part, part)
        term = contract_cols(gd[z], wg[span, :]) + contract_cols(ud[z], wu[span, :])
        term = term.astype(terms.dtype)
        terms[..., span] = term.reshape(terms.shape[:-1] + (part,))
        if n == 0:
            hop(1, 0)
        if n == 2:
            relay(0, 0)

    def sum_copy(kind, slot, src, dst, device):
        return pltpu.make_async_remote_copy(
            src_ref=src, dst_ref=dst, send_sem=sum_send.at[kind, slot],
            recv_sem=sum_recv.at[kind, slot], device_id=device, device_id_type=MESH,
        )

    swaps = [put(None, sum_copy(0, j, terms.at[j, 1 - core], got.at[j], other)) for j in range(chips)]
    hop(0, 1)
    relay(1, 0)

    def reduce_first():
        for j in range(chips):
            swaps[j].wait_recv()
            pair = terms[j, core].astype(jnp.float32) + got[j].astype(jnp.float32)
            sums[j] = pair.astype(sums.dtype)
        spread = []
        for ahead in range(1, chips):
            there, device = peer(ahead)
            spread.append(put(None, sum_copy(1, ahead, sums.at[there], landed.at[ahead], device)))
        return spread

    done = out.at[chip, core]

    def reduce_second(spread):
        total = terms[chip, core].astype(jnp.float32) + got[chip].astype(jnp.float32)
        for ahead in range(1, chips):
            spread[ahead - 1].wait_recv()
            total = total + landed[ahead].astype(jnp.float32)
        out[chip, core] = total.astype(out.dtype)
        share = [put(None, sum_copy(2, ahead, done, done, peer(ahead)[1])) for ahead in range(1, chips)]
        relays = [put(None, sum_copy(3, 0, done, done, other))]
        return share, relays

    def reduce_third(share, relays):
        for ahead in range(1, chips):
            share[ahead - 1].wait_recv()
            source = out.at[(chip + chips - ahead) % chips, core]
            relays.append(put(None, sum_copy(3, ahead, source, source, other)))

    fewer = jnp.minimum(z, reps - 1 - z)

    def order(turn):
        step = jnp.where(turn < 2 * fewer, turn // 2, turn - fewer)
        low = jnp.where(turn < 2 * fewer, turn % 2 == 0, z > reps - 1 - z)
        return jnp.where(low, z - 1 - step, z + 1 + step)

    keep_cols(0, z)
    keep_cols(1, z)
    share = relays = spread = None
    for turn in range(reps - 1):
        block = order(turn)
        complete(0, block)
        keep_cols(0, block)
        for n, (at, size) in enumerate(pieces):
            pre(block, at, size)
        if turn == 0:
            spread = reduce_first()
        if turn == 1:
            share, relays = reduce_second(spread)
        if turn + 1 < reps - 1:
            hop(1, turn + 1)
            relay(0, turn + 1)
        complete(1, block)
        keep_cols(1, block)
        for n, (at, size) in enumerate(pieces):
            deltas(block, at, size)
        if turn + 2 < reps - 1:
            hop(0, turn + 2)
        if turn + 1 < reps - 1:
            relay(1, turn + 1)
        if turn == 1:
            reduce_third(share, relays)
    for copy in relays:
        copy.wait_recv()
    for condition, copy in started:
        if condition is None:
            copy.wait_send()
        else:
            guarded(condition, copy.wait_send)


def fused(reps, chips, across, inputs, cotangent, w_gate, w_upward, w_down):
    rows, width = inputs.shape
    hidden = w_gate.shape[1]
    cols = width // reps
    kind = inputs.dtype
    piece = (rows // (2 * chips), width)
    vmem = pl.BlockSpec(memory_space=pltpu.VMEM)
    anywhere = pl.BlockSpec(memory_space=pl.ANY)
    count = len(chunks_of(hidden, 512))
    wide = jax.ShapeDtypeStruct((reps, rows, hidden), kind)
    slim = jax.ShapeDtypeStruct((reps, rows, cols), kind)
    total, hid, gd, ud, xc, cc = pl.pallas_call(
        functools.partial(fused_kernel, reps, chips, across),
        out_shape=(jax.ShapeDtypeStruct((chips, 2) + piece, kind), wide, wide, wide, slim, slim),
        in_specs=[anywhere] * 5,
        out_specs=(vmem,) * 6,
        scratch_shapes=[
            pltpu.VMEM((reps, rows, width), kind),
            pltpu.VMEM((reps, rows, width), kind),
            pltpu.VMEM((width, hidden), kind),
            pltpu.VMEM((width, hidden), kind),
            pltpu.VMEM((hidden, width), kind),
            pltpu.VMEM((rows, hidden), jnp.float32),
            pltpu.VMEM((rows, hidden), jnp.float32),
            pltpu.VMEM((chips, 2) + piece, kind),
            pltpu.VMEM((chips,) + piece, kind),
            pltpu.VMEM((chips,) + piece, kind),
            pltpu.VMEM((chips,) + piece, kind),
            pltpu.SemaphoreType.DMA((10, reps)),
            pltpu.SemaphoreType.DMA((8, reps)),
            pltpu.SemaphoreType.DMA((4, chips)),
            pltpu.SemaphoreType.DMA((4, chips)),
            pltpu.SemaphoreType.DMA((2,)),
            pltpu.SemaphoreType.DMA((count, 3)),
        ],
        compiler_params=pltpu.CompilerParams(
            collective_id=2, has_side_effects=True, vmem_limit_bytes=63 * 2**20
        ),
        name="gather_compute",
    )(inputs, cotangent, w_gate, w_upward, w_down)
    return total.reshape(rows, width), [a.reshape(reps * rows, -1) for a in (hid, gd, ud, xc, cc)]


def weights_kernel(tall, wide_rows, hid, gd, ud, xc, cc, total, g_gate, g_up, g_down, g_in, stage, stage_down, sems, down_sems, in_sem):
    whole = pltpu.make_async_copy(total, g_in, in_sem)
    whole.start()
    pending = [None] * stage.shape[0]
    turn = 0
    for delta, target in ((gd, g_gate), (ud, g_up)):
        for at, size in chunks_of(xc.shape[1], tall):
            slot = turn % len(pending)
            if pending[slot] is not None:
                pending[slot].wait()
            span = pl.ds(at, size)
            stage[slot, :size] = contract_rows(xc[:, span], delta[...])
            pending[slot] = pltpu.make_async_copy(stage.at[slot, pl.ds(0, size)], target.at[span], sems.at[slot])
            pending[slot].start()
            turn += 1
    later = [None] * stage_down.shape[0]
    turn = 0
    for at, size in chunks_of(hid.shape[1], wide_rows):
        slot = turn % len(later)
        if later[slot] is not None:
            later[slot].wait()
        span = pl.ds(at, size)
        stage_down[slot, :size] = contract_rows(hid[:, span], cc[...])
        later[slot] = pltpu.make_async_copy(stage_down.at[slot, pl.ds(0, size)], g_down.at[span], down_sems.at[slot])
        later[slot].start()
        turn += 1
    for copy in pending + later:
        if copy is not None:
            copy.wait()
    whole.wait()


def weight_gradients(total, hid, gd, ud, xc, cc):
    hidden, cols = hid.shape[1], xc.shape[1]
    vmem = pl.BlockSpec(memory_space=pltpu.VMEM)
    anywhere = pl.BlockSpec(memory_space=pl.ANY)
    up = jax.ShapeDtypeStruct((cols, hidden), jnp.float32)
    down = jax.ShapeDtypeStruct((hidden, cols), jnp.float32)
    tall, wide_rows, slots = 256, 384, 3
    return pl.pallas_call(
        functools.partial(weights_kernel, tall, wide_rows),
        out_shape=(up, up, down, jax.ShapeDtypeStruct(total.shape, total.dtype)),
        in_specs=[vmem] * 6,
        out_specs=(anywhere,) * 4,
        scratch_shapes=[
            pltpu.VMEM((slots, tall, hidden), jnp.float32),
            pltpu.VMEM((slots, wide_rows, cols), jnp.float32),
            pltpu.SemaphoreType.DMA((slots,)),
            pltpu.SemaphoreType.DMA((slots,)),
            pltpu.SemaphoreType.DMA,
        ],
        compiler_params=pltpu.CompilerParams(vmem_limit_bytes=40 * 2**20),
        name="weight_gradients",
    )(hid, gd, ud, xc, cc, total)


def fits(reps, chips, across, inputs, w_gate):
    rows, width = inputs.shape
    hidden = w_gate.shape[1]
    size = inputs.dtype.itemsize
    need = size * (3 * width * hidden + 2 * reps * rows * width + 3 * reps * rows * hidden)
    aligned = hidden % 128 == 0 and width % (128 * reps) == 0 and rows % 64 == 0
    return aligned and chips == 4 and across == 2 and need < 52 * 2**20


def local(reps, chips, across, inputs, cotangent, w_gate, w_upward, w_down):
    rows, width = inputs.shape
    if fits(reps, chips, across, inputs, w_gate):
        total, parts = fused(reps, chips, across, inputs, cotangent, w_gate, w_upward, w_down)
        grad_gate, grad_upward, grad_down, grad_input = weight_gradients(total, *parts)
        return (grad_input, grad_gate, grad_upward, grad_down)
    all_inputs, all_cotangent = gather(reps, inputs, cotangent)

    gate_pre = jnp.dot(all_inputs, w_gate, preferred_element_type=jnp.float32)
    up_pre = jnp.dot(all_inputs, w_upward, preferred_element_type=jnp.float32)
    sigmoid_gate = jax.nn.sigmoid(gate_pre)
    activated = gate_pre * sigmoid_gate
    hidden = (activated * up_pre).astype(jnp.bfloat16)
    hidden_grad = contract_cols(all_cotangent, w_down)
    gate_delta = (
        hidden_grad * up_pre * sigmoid_gate * (1.0 + gate_pre * (1.0 - sigmoid_gate))
    ).astype(jnp.bfloat16)
    up_delta = (hidden_grad * activated).astype(jnp.bfloat16)

    z = lax.axis_index("rep")
    own_gate = lax.dynamic_slice_in_dim(gate_delta, z * rows, rows, 0)
    own_up = lax.dynamic_slice_in_dim(up_delta, z * rows, rows, 0)
    terms = contract_cols(own_gate, w_gate) + contract_cols(own_up, w_upward)
    grad_input = plane_sum(chips, across, terms.astype(jnp.bfloat16))

    cols = width // reps
    input_cols = lax.dynamic_slice_in_dim(all_inputs, z * cols, cols, 1)
    cotangent_cols = lax.dynamic_slice_in_dim(all_cotangent, z * cols, cols, 1)
    grad_gate = contract_rows(input_cols, gate_delta)
    grad_upward = contract_rows(input_cols, up_delta)
    grad_down = contract_rows(hidden, cotangent_cols)
    return (grad_input, grad_gate, grad_upward, grad_down)


def solution(mesh):
    across = mesh.shape["tp"] // 2
    chips = mesh.shape["fs"] * across
    in_specs = (
        P("rep", None),
        P("rep", None),
        P(None, PLANE),
        P(None, PLANE),
        P(PLANE, None),
    )
    out_specs = (
        P("rep", None),
        P("rep", PLANE),
        P("rep", PLANE),
        P(PLANE, "rep"),
    )
    body = functools.partial(local, mesh.shape["rep"], chips, across)
    return jax.shard_map(body, mesh=mesh, in_specs=in_specs, out_specs=out_specs, check_vma=False)
```

```python
import functools

import jax
import jax.numpy as jnp
from jax import lax
from jax.experimental import pallas as pl
from jax.experimental.pallas import tpu as pltpu
from jax.sharding import PartitionSpec as P

PLANE = ("fs", "tp")
MESH = pl.DeviceIdType.MESH
STREAM = (256, 256, 512, 384)
BLOCK = (512, 512, 384)
FLIGHT = 4


def contract_rows(left, right):
    return lax.dot_general(
        left, right, (((0,), (0,)), ((), ())), preferred_element_type=jnp.float32
    )


def contract_cols(left, right):
    return lax.dot_general(
        left, right, (((1,), (1,)), ((), ())), preferred_element_type=jnp.float32
    )


def greet(neighbours):
    barrier = pltpu.get_barrier_semaphore()
    for device in neighbours:
        pl.semaphore_signal(barrier, inc=1, device_id=device, device_id_type=MESH)
    pl.semaphore_wait(barrier, len(neighbours))


def gather_kernel(reps, x_ref, c_ref, all_x, all_c, send, recv, own_sem):
    z, y, t = lax.axis_index("rep"), lax.axis_index("fs"), lax.axis_index("tp")
    x, core = t // 2, t % 2
    half = (x + y) % 2
    mine = 2 * half + core
    across = 2 * (1 - half) + core
    up, down = (z + 1) % reps, (z + reps - 1) % reps
    to_up, to_down = (up, y, t), (down, y, t)
    x_near = (z, y, 2 * (x + 1 - 2 * (x % 2)) + core)
    y_near = (z, y + 1 - 2 * (y % 2), t)
    other = (z, y, 2 * x + 1 - core)
    greet((to_up, to_down, x_near, y_near, other))

    started = []

    def put(kind, step, src, dst, device):
        copy = pltpu.make_async_remote_copy(
            src_ref=src, dst_ref=dst, send_sem=send.at[kind, step],
            recv_sem=recv.at[kind, step], device_id=device, device_id_type=MESH,
        )
        copy.start()
        started.append(copy)
        return copy

    ring = [
        put(0, 0, x_ref.at[mine], all_x.at[z, mine], to_up),
        put(1, 0, c_ref.at[mine], all_c.at[z, mine], to_down),
    ]
    keep = [
        pltpu.make_async_copy(x_ref, all_x.at[z], own_sem.at[0]),
        pltpu.make_async_copy(c_ref, all_c.at[z], own_sem.at[1]),
    ]
    for copy in keep:
        copy.start()

    last = []

    def relay(sides, step, bx, bc):
        sides[0].wait_recv()
        last.append(put(6, step, all_x.at[bx, across], all_x.at[bx, across], other))
        sides[1].wait_recv()
        last.append(put(7, step, all_c.at[bc, across], all_c.at[bc, across], other))

    before = None
    for step in range(reps - 1):
        bx, bc = (z + reps - 1 - step) % reps, (z + 1 + step) % reps
        got_x, got_c = all_x.at[bx, mine], all_c.at[bc, mine]
        following = []
        ring[0].wait_recv()
        if step < reps - 2:
            following.append(put(0, step + 1, got_x, got_x, to_up))
        side_x = put(2, step, got_x, got_x, x_near)
        last.append(put(4, step, got_x, got_x, other))
        ring[1].wait_recv()
        if step < reps - 2:
            following.append(put(1, step + 1, got_c, got_c, to_down))
        side_c = put(3, step, got_c, got_c, y_near)
        last.append(put(5, step, got_c, got_c, other))
        if before is not None:
            relay(*before)
        before = ((side_x, side_c), step, bx, bc)
        ring = following
    relay(*before)
    for copy in last:
        copy.wait_recv()
    for copy in started:
        copy.wait_send()
    for copy in keep:
        copy.wait()


def gather(reps, inputs, cotangent):
    rows, width = inputs.shape
    quarter = (4, rows // 4, width)
    whole = jax.ShapeDtypeStruct((reps,) + quarter, inputs.dtype)
    vmem = pl.BlockSpec(memory_space=pltpu.VMEM)
    pair = pl.pallas_call(
        functools.partial(gather_kernel, reps),
        out_shape=(whole, whole),
        in_specs=[vmem, vmem],
        out_specs=(vmem, vmem),
        scratch_shapes=[
            pltpu.SemaphoreType.DMA((8, reps - 1)),
            pltpu.SemaphoreType.DMA((8, reps - 1)),
            pltpu.SemaphoreType.DMA((2,)),
        ],
        compiler_params=pltpu.CompilerParams(
            collective_id=0, has_side_effects=True, vmem_limit_bytes=60 * 2**20
        ),
        name="token_gather",
    )(inputs.reshape(quarter), cotangent.reshape(quarter))
    return [a.reshape(reps * rows, width) for a in pair]


def reduce_kernel(chips, across, terms, out, got, sums, landed, send, recv):
    z, y, t = lax.axis_index("rep"), lax.axis_index("fs"), lax.axis_index("tp")
    core = t % 2
    chip = y * across + t // 2
    other = (z, y, t + 1 - 2 * core)

    def peer(ahead):
        there = (chip + ahead) % chips
        return there, (z, there // across, 2 * (there % across) + core)

    greet([other] + [peer(ahead)[1] for ahead in range(1, chips)])

    def put(kind, slot, src, dst, device):
        copy = pltpu.make_async_remote_copy(
            src_ref=src, dst_ref=dst, send_sem=send.at[kind, slot],
            recv_sem=recv.at[kind, slot], device_id=device, device_id_type=MESH,
        )
        copy.start()
        return copy

    swaps = [put(0, j, terms.at[j, 1 - core], got.at[j], other) for j in range(chips)]
    for j in range(chips):
        swaps[j].wait_recv()
        pair = terms[j, core].astype(jnp.float32) + got[j].astype(jnp.float32)
        sums[j] = pair.astype(sums.dtype)
    spread = []
    for ahead in range(1, chips):
        there, device = peer(ahead)
        spread.append(put(1, ahead, sums.at[there], landed.at[ahead], device))
    total = terms[chip, core].astype(jnp.float32) + got[chip].astype(jnp.float32)
    for ahead in range(1, chips):
        spread[ahead - 1].wait_recv()
        total = total + landed[ahead].astype(jnp.float32)
    out[chip, core] = total.astype(out.dtype)
    done = out.at[chip, core]
    share = [put(2, ahead, done, done, peer(ahead)[1]) for ahead in range(1, chips)]
    relays = [put(3, 0, done, done, other)]
    for ahead in range(1, chips):
        share[ahead - 1].wait_recv()
        source = out.at[(chip + chips - ahead) % chips, core]
        relays.append(put(3, ahead, source, source, other))
    for copy in relays:
        copy.wait_recv()
    for copy in swaps + spread + share + relays:
        copy.wait_send()


def plane_sum(chips, across, terms):
    rows, width = terms.shape
    piece = (rows // (2 * chips), width)
    vmem = pl.BlockSpec(memory_space=pltpu.VMEM)
    total = pl.pallas_call(
        functools.partial(reduce_kernel, chips, across),
        out_shape=jax.ShapeDtypeStruct((chips, 2) + piece, terms.dtype),
        in_specs=[vmem],
        out_specs=vmem,
        scratch_shapes=[
            pltpu.VMEM((chips,) + piece, terms.dtype),
            pltpu.VMEM((chips,) + piece, terms.dtype),
            pltpu.VMEM((chips,) + piece, terms.dtype),
            pltpu.SemaphoreType.DMA((4, chips)),
            pltpu.SemaphoreType.DMA((4, chips)),
        ],
        compiler_params=pltpu.CompilerParams(
            collective_id=1, has_side_effects=True, vmem_limit_bytes=48 * 2**20
        ),
        name="plane_sum",
    )(terms.reshape((chips, 2) + piece))
    return total.reshape(rows, width)


def chunks_of(total, widths):
    spans, at = [], 0
    for width in widths:
        if at < total:
            spans.append((at, min(width, total - at)))
            at += width
    while at < total:
        spans.append((at, min(widths[-1], total - at)))
        at += widths[-1]
    return spans


def fused_kernel(
    reps, chips, across, x_hbm, c_hbm, wg_hbm, wu_hbm, wd_hbm,
    out, hid, gd, ud, xc, cc,
    all_x, all_c, wg, wu, wd, gpre, upre, got, landed,
    send, recv, sum_send, sum_recv, local_sem, weight_sem,
):
    z, y, t = lax.axis_index("rep"), lax.axis_index("fs"), lax.axis_index("tp")
    x, core = t // 2, t % 2
    rows, width = all_x.shape[1:]
    hidden = wg.shape[1]
    cols = width // reps
    chip = y * across + x
    x_chip, y_chip = y * across + 1 - x, (1 - y) * across + x
    far_chip = (1 - y) * across + 1 - x
    x_near, y_near = (z, y, 2 * (1 - x) + core), (z, 1 - y, t)
    other = (z, y, 2 * x + 1 - core)
    near = (z, jnp.where(core == 0, y, 1 - y), jnp.where(core == 0, 2 * (1 - x) + core, t))
    crosswise = (z, jnp.where(core == 0, 1 - y, y), jnp.where(core == 0, t, 2 * (1 - x) + core))
    half = (x + y) % 2

    def peer(ahead):
        there = (chip + ahead) % chips
        return there, (z, there // across, 2 * (there % across) + core)

    def part_of(parts, index):
        size = rows // parts
        return pl.ds(pl.multiple_of(index * size, size), size)

    def x_part(of_chip, of_core):
        return part_of(8, 2 * of_chip + of_core)

    def c_part(of_half, of_core):
        return part_of(4, 2 * of_half + of_core)

    local = [
        pltpu.make_async_copy(x_hbm, all_x.at[0], local_sem.at[0]),
        pltpu.make_async_copy(c_hbm, all_c.at[0], local_sem.at[1]),
    ]
    for copy in local:
        copy.start()
    stream = chunks_of(hidden, STREAM)
    weights = []
    for n, (at, size) in enumerate(stream):
        span = pl.ds(at, size)
        weights += [
            pltpu.make_async_copy(wg_hbm.at[:, span], wg.at[:, span], weight_sem.at[n, 0]),
            pltpu.make_async_copy(wu_hbm.at[:, span], wu.at[:, span], weight_sem.at[n, 1]),
            pltpu.make_async_copy(wd_hbm.at[span], wd.at[span], weight_sem.at[n, 2]),
        ]
    for copy in weights[:FLIGHT]:
        copy.start()

    def weight_ready(n):
        weights[n].wait()
        if n + FLIGHT < len(weights):
            weights[n + FLIGHT].start()

    greet(
        [((z + 1) % reps, y, t), ((z + reps - 1) % reps, y, t), other]
        + [peer(ahead)[1] for ahead in range(1, chips)]
    )

    def slot_of(level, block):
        step = jnp.where(block < level, level - block, block - level) - 1
        fewer = jnp.minimum(level, reps - 1 - level)
        paired = 2 * step + jnp.where(block < level, 0, 1)
        return 1 + jnp.where(step < fewer, paired, step + fewer)

    def make(kind, slot, src, dst, device, sender=None, there=None):
        return pltpu.make_async_remote_copy(
            src_ref=src, dst_ref=dst, send_sem=send.at[kind if sender is None else sender, slot],
            recv_sem=recv.at[kind, slot if there is None else there],
            device_id=device, device_id_type=MESH,
        )

    def pass_on(buffer, kind, slot, part, device):
        piece = buffer.at[slot, part]
        return make(kind, slot, piece, piece, device)

    def hop_on(buffer, kind, slot, part, device, there):
        return make(kind, slot, buffer.at[slot, part], buffer.at[there, part], device, None, there)

    above, below = jnp.minimum(z + 1, reps - 1), jnp.maximum(z - 1, 0)
    up, down = (above, y, t), (below, y, t)

    def first_sends():
        sends = []
        for kind, src, buffer, part in (
            (0, x_hbm, all_x, x_part(chip, core)), (8, c_hbm, all_c, c_part(half, core))
        ):
            for wanted, device, level, sender in (
                (z < reps - 1, up, above, kind), (z > 0, down, below, 12 + kind // 8)
            ):
                there = slot_of(level, z)
                copy = make(kind, 0, src.at[part], buffer.at[there, part], device, sender, there)
                sends.append((wanted, copy))
        return sends

    def sides(step):
        low, high = z - 1 - step, z + 1 + step
        from_low, from_high = jnp.maximum(low, 0), jnp.minimum(high, reps - 1)
        return (
            (low >= 0, slot_of(z, from_low), up, slot_of(above, from_low), (low >= 0) & (z < reps - 1)),
            (high < reps, slot_of(z, from_high), down, slot_of(below, from_high), (high < reps) & (z > 0)),
        )

    def hops(buffer, kind, part, step):
        for valid, slot, onward, there, passes in sides(step):
            yield valid, pass_on(buffer, kind, slot, part, other), passes, hop_on(buffer, kind, slot, part, onward, there)

    def hop(array, step):
        buffer, kind, part = ((all_x, 0, x_part(chip, core)), (all_c, 8, c_part(half, core)))[array]
        for valid, arrived, passes, onward in hops(buffer, kind, part, step):
            pl.when(valid)(arrived.wait_recv)
            pl.when(passes)(onward.start)

    beside, across_y, opposite = x_part(x_chip, core), x_part(y_chip, core), x_part(far_chip, core)
    turned = part_of(8, 2 * jnp.where(core == 0, x_chip, y_chip) + core)

    def near_x(slot):
        part = x_part(chip, core)
        return [
            pass_on(all_x, 1, slot, part, x_near), pass_on(all_x, 2, slot, part, y_near),
            pass_on(all_x, 4, slot, part, other),
        ]

    def spread_x(slot):
        return [
            pass_on(all_x, 3, slot, turned, crosswise), pass_on(all_x, 5, slot, beside, other),
            pass_on(all_x, 6, slot, across_y, other),
        ]

    def last_x(slot):
        return [pass_on(all_x, 7, slot, opposite, other)]

    def near_c(slot):
        part = c_part(half, core)
        return [pass_on(all_c, 9, slot, part, near), pass_on(all_c, 10, slot, part, other)]

    def last_c(slot):
        return [pass_on(all_c, 11, slot, c_part(1 - half, core), other)]

    awaited = {
        near_x: (), near_c: (), spread_x: ((1, beside), (2, across_y)), last_x: ((3, opposite),),
        last_c: ((9, c_part(1 - half, core)),),
    }

    def serve(service, slot):
        buffer = all_c if service in (near_c, last_c) else all_x
        for kind, part in awaited[service]:
            pass_on(buffer, kind, slot, part, other).wait_recv()
        for copy in service(slot):
            copy.start()

    def complete_x(slot):
        for kind in range(4, 8):
            pass_on(all_x, kind, slot, x_part(chip, core), other).wait_recv()
        keep_cols(all_x, xc, slot)

    def complete_c(slot):
        for kind in range(10, 12):
            pass_on(all_c, kind, slot, c_part(half, core), other).wait_recv()
        keep_cols(all_c, cc, slot)

    def pre(slot, place, at, size):
        span, held = pl.ds(at, size), pl.ds(place * rows, rows)
        tokens = all_x[slot]
        gpre[held, span] = jnp.dot(tokens, wg[:, span], preferred_element_type=jnp.float32)
        upre[held, span] = jnp.dot(tokens, wu[:, span], preferred_element_type=jnp.float32)

    def deltas(slot, count, at, size):
        span, held, slots = pl.ds(at, size), pl.ds(0, count * rows), pl.ds(slot, count)
        tokens = all_c[slots].reshape(count * rows, width)
        grad = contract_cols(tokens, wd[span, :])
        gate, lift = gpre[held, span], upre[held, span]
        sig = jax.nn.sigmoid(gate)
        act = gate * sig
        shape = (count, rows, size)
        hid[slots, :, span] = (act * lift).astype(hid.dtype).reshape(shape)
        gate_grad = grad * lift * sig * (1.0 + gate * (1.0 - sig))
        gd[slots, :, span] = gate_grad.astype(gd.dtype).reshape(shape)
        ud[slots, :, span] = (grad * act).astype(ud.dtype).reshape(shape)

    def keep_cols(buffer, kept, slot):
        span = pl.ds(pl.multiple_of(z * cols, cols), cols)
        kept[slot] = buffer[slot, :, span]

    small = rows // (2 * chips)

    def term(piece, of_core):
        return all_c.at[0, part_of(2 * chips, 2 * piece + of_core)]

    def pair_sum(ahead):
        return all_x.at[0, pl.ds((ahead - 1) * small, small)]

    def sum_copy(kind, slot, src, dst, device):
        return pltpu.make_async_remote_copy(
            src_ref=src, dst_ref=dst, send_sem=sum_send.at[kind, slot],
            recv_sem=sum_recv.at[kind, slot], device_id=device, device_id_type=MESH,
        )

    def swaps():
        return [sum_copy(0, j, term(j, 1 - core), got.at[j], other) for j in range(chips)]

    def spread():
        return [
            sum_copy(1, ahead, pair_sum(ahead), landed.at[ahead - 1], peer(ahead)[1])
            for ahead in range(1, chips)
        ]

    def share():
        done = out.at[chip, core]
        return [sum_copy(2, ahead, done, done, peer(ahead)[1]) for ahead in range(1, chips)]

    def relays():
        sources = [out.at[(chip + chips - ahead) % chips, core] for ahead in range(chips)]
        return [sum_copy(3, ahead, source, source, other) for ahead, source in enumerate(sources)]

    def reduce_first():
        for copy in swaps():
            copy.wait_recv()
        for ahead in range(1, chips):
            there = peer(ahead)[0]
            pair = term(there, core)[...].astype(jnp.float32) + got[there].astype(jnp.float32)
            pair_sum(ahead)[...] = pair.astype(got.dtype)
        for ahead, copy in enumerate(spread(), 1):
            pl.when(peer(ahead)[0] != far_chip)(copy.start)

    def diagonal():
        for ahead, copy in enumerate(spread(), 1):
            pl.when(peer(ahead)[0] == far_chip)(copy.start)

    def reduce_second():
        total = term(chip, core)[...].astype(jnp.float32) + got[chip].astype(jnp.float32)
        for ahead, copy in enumerate(spread()):
            copy.wait_recv()
            total = total + landed[ahead].astype(jnp.float32)
        out[chip, core] = total.astype(out.dtype)
        for copy in share():
            copy.start()
        relays()[0].start()

    def reduce_third():
        for copy, onward in zip(share(), relays()[1:]):
            copy.wait_recv()
            onward.start()

    for condition, copy in first_sends():
        pl.when(condition)(copy.start)
    for copy in local:
        copy.wait()
    keep_cols(all_x, xc, 0)
    keep_cols(all_c, cc, 0)
    slots = {
        (0, 1): ((hop, 0, 0), (serve, near_x, 1)),
        (1, 2): ((serve, spread_x, 1), (hop, 1, 0), (serve, near_c, 1)),
        (1, 3): ((hop, 0, 1), (serve, near_x, 2)),
        (2, 0): ((serve, last_x, 1),),
        (2, 2): ((serve, last_c, 1), (hop, 1, 1), (serve, near_c, 2)),
        (2, 3): ((serve, spread_x, 2),),
        (3, 0): ((hop, 0, 2), (serve, near_x, 3)),
        (3, 2): ((serve, last_x, 2),),
        (4, 0): ((serve, last_c, 2),),
        (4, 1): ((serve, spread_x, 3), (diagonal,)),
        (4, 2): ((hop, 1, 2), (serve, near_c, 3)),
        (5, 2): ((serve, last_x, 3),),
        (6, 1): ((serve, last_c, 3), (reduce_second,)),
    }

    def at_slot(phase, n):
        for action, *details in slots.get((phase, n), ()):
            action(*details)

    for n, (at, size) in enumerate(stream):
        weight_ready(3 * n)
        weight_ready(3 * n + 1)
        pre(0, 0, at, size)
        at_slot(0, n)
        weight_ready(3 * n + 2)
        deltas(0, 1, at, size)
        at_slot(1, n)

    part = width // 4
    for n in range(4):
        span = pl.ds(n * part, part)
        total = contract_cols(gd[0], wg[span, :]) + contract_cols(ud[0], wu[span, :])
        all_c[0, :, span] = total.astype(all_c.dtype)
        at_slot(2, n)
    for copy in swaps():
        copy.start()

    blocks = chunks_of(hidden, BLOCK)
    complete_x(1)
    for n, (at, size) in enumerate(blocks):
        pre(1, 0, at, size)
        at_slot(3, n)
        if n == 1:
            reduce_first()
    complete_c(1)
    for n, (at, size) in enumerate(blocks):
        deltas(1, 1, at, size)
        at_slot(4, n)
    complete_x(2)
    for n, (at, size) in enumerate(blocks):
        pre(2, 0, at, size)
        at_slot(5, n)
    complete_x(3)
    for n, (at, size) in enumerate(blocks):
        pre(3, 1, at, size)
        at_slot(6, n)
    complete_c(2)
    complete_c(3)
    for n, (at, size) in enumerate(blocks):
        deltas(2, 2, at, size)
    reduce_third()
    for copy in relays():
        copy.wait_recv()
    for condition, copy in first_sends():
        pl.when(condition)(copy.wait_send)
    for copy in swaps() + spread() + share() + relays():
        copy.wait_send()

    for slot in range(1, reps):
        for service in (near_x, spread_x, last_x, near_c, last_c):
            for copy in service(slot):
                copy.wait_send()
    for step in range(reps - 1):
        for buffer, kind, part in ((all_x, 0, x_part(chip, core)), (all_c, 8, c_part(half, core))):
            for _, _, passes, onward in hops(buffer, kind, part, step):
                pl.when(passes)(onward.wait_send)


def fused(reps, chips, across, inputs, cotangent, w_gate, w_upward, w_down):
    rows, width = inputs.shape
    hidden = w_gate.shape[1]
    cols = width // reps
    kind = inputs.dtype
    piece = (rows // (2 * chips), width)
    vmem = pl.BlockSpec(memory_space=pltpu.VMEM)
    anywhere = pl.BlockSpec(memory_space=pl.ANY)
    count = len(chunks_of(hidden, STREAM))
    wide = jax.ShapeDtypeStruct((reps, rows, hidden), kind)
    slim = jax.ShapeDtypeStruct((reps, rows, cols), kind)
    total, hid, gd, ud, xc, cc = pl.pallas_call(
        functools.partial(fused_kernel, reps, chips, across),
        out_shape=(jax.ShapeDtypeStruct((chips, 2) + piece, kind), wide, wide, wide, slim, slim),
        in_specs=[pl.BlockSpec(memory_space=pltpu.HBM)] * 5,
        out_specs=(vmem,) * 6,
        scratch_shapes=[
            pltpu.VMEM((reps, rows, width), kind),
            pltpu.VMEM((reps, rows, width), kind),
            pltpu.VMEM((width, hidden), kind),
            pltpu.VMEM((width, hidden), kind),
            pltpu.VMEM((hidden, width), kind),
            pltpu.VMEM((2 * rows, hidden), jnp.float32),
            pltpu.VMEM((2 * rows, hidden), jnp.float32),
            pltpu.VMEM((chips,) + piece, kind),
            pltpu.VMEM((chips - 1,) + piece, kind),
            pltpu.SemaphoreType.DMA((14, reps)),
            pltpu.SemaphoreType.DMA((12, reps)),
            pltpu.SemaphoreType.DMA((4, chips)),
            pltpu.SemaphoreType.DMA((4, chips)),
            pltpu.SemaphoreType.DMA((2,)),
            pltpu.SemaphoreType.DMA((count, 3)),
        ],
        compiler_params=pltpu.CompilerParams(
            collective_id=2, has_side_effects=True, vmem_limit_bytes=46 * 2**20 + 704 * 2**10
        ),
        name="gather_compute",
    )(*(pltpu.with_memory_space_constraint(a, pltpu.HBM) for a in (inputs, cotangent, w_gate, w_upward, w_down)))
    return total.reshape(rows, width), [a.reshape(reps * rows, -1) for a in (hid, gd, ud, xc, cc)]


def weights_kernel(tall, wide_rows, hid, gd, ud, xc, cc, total, g_gate, g_up, g_down, g_in, stage, stage_down, sems, down_sems, in_sem):
    whole = pltpu.make_async_copy(total, g_in, in_sem)
    whole.start()
    pending = [None] * stage.shape[0]
    turn = 0
    for delta, target in ((gd, g_gate), (ud, g_up)):
        for at, size in chunks_of(xc.shape[1], (tall,)):
            slot = turn % len(pending)
            if pending[slot] is not None:
                pending[slot].wait()
            span = pl.ds(at, size)
            stage[slot, :size] = contract_rows(xc[:, span], delta[...])
            pending[slot] = pltpu.make_async_copy(stage.at[slot, pl.ds(0, size)], target.at[span], sems.at[slot])
            pending[slot].start()
            turn += 1
    later = [None] * stage_down.shape[0]
    turn = 0
    for at, size in chunks_of(hid.shape[1], (wide_rows,)):
        slot = turn % len(later)
        if later[slot] is not None:
            later[slot].wait()
        span = pl.ds(at, size)
        stage_down[slot, :size] = contract_rows(hid[:, span], cc[...])
        later[slot] = pltpu.make_async_copy(stage_down.at[slot, pl.ds(0, size)], g_down.at[span], down_sems.at[slot])
        later[slot].start()
        turn += 1
    for copy in pending + later:
        if copy is not None:
            copy.wait()
    whole.wait()


def weight_gradients(total, hid, gd, ud, xc, cc):
    hidden, cols = hid.shape[1], xc.shape[1]
    vmem = pl.BlockSpec(memory_space=pltpu.VMEM)
    anywhere = pl.BlockSpec(memory_space=pl.ANY)
    up = jax.ShapeDtypeStruct((cols, hidden), jnp.float32)
    down = jax.ShapeDtypeStruct((hidden, cols), jnp.float32)
    tall, wide_rows, slots = 256, 384, 3
    return pl.pallas_call(
        functools.partial(weights_kernel, tall, wide_rows),
        out_shape=(up, up, down, jax.ShapeDtypeStruct(total.shape, total.dtype)),
        in_specs=[vmem] * 6,
        out_specs=(anywhere,) * 4,
        scratch_shapes=[
            pltpu.VMEM((slots, tall, hidden), jnp.float32),
            pltpu.VMEM((slots, wide_rows, cols), jnp.float32),
            pltpu.SemaphoreType.DMA((slots,)),
            pltpu.SemaphoreType.DMA((slots,)),
            pltpu.SemaphoreType.DMA,
        ],
        compiler_params=pltpu.CompilerParams(vmem_limit_bytes=20 * 2**20),
        name="weight_gradients",
    )(hid, gd, ud, xc, cc, total)


def fits(reps, chips, across, inputs, w_gate):
    rows, width = inputs.shape
    hidden = w_gate.shape[1]
    size = inputs.dtype.itemsize
    need = size * (3 * width * hidden + 2 * reps * rows * width + 3 * reps * rows * hidden)
    aligned = hidden % 128 == 0 and width % (128 * reps) == 0 and rows % 128 == 0
    return aligned and chips == 4 and across == 2 and reps == 4 and need < 52 * 2**20


def local(reps, chips, across, inputs, cotangent, w_gate, w_upward, w_down):
    rows, width = inputs.shape
    if fits(reps, chips, across, inputs, w_gate):
        total, parts = fused(reps, chips, across, inputs, cotangent, w_gate, w_upward, w_down)
        grad_gate, grad_upward, grad_down, grad_input = weight_gradients(total, *parts)
        return (grad_input, grad_gate, grad_upward, grad_down)
    all_inputs, all_cotangent = gather(reps, inputs, cotangent)

    gate_pre = jnp.dot(all_inputs, w_gate, preferred_element_type=jnp.float32)
    up_pre = jnp.dot(all_inputs, w_upward, preferred_element_type=jnp.float32)
    sigmoid_gate = jax.nn.sigmoid(gate_pre)
    activated = gate_pre * sigmoid_gate
    hidden = (activated * up_pre).astype(jnp.bfloat16)
    hidden_grad = contract_cols(all_cotangent, w_down)
    gate_delta = (
        hidden_grad * up_pre * sigmoid_gate * (1.0 + gate_pre * (1.0 - sigmoid_gate))
    ).astype(jnp.bfloat16)
    up_delta = (hidden_grad * activated).astype(jnp.bfloat16)

    z = lax.axis_index("rep")
    own_gate = lax.dynamic_slice_in_dim(gate_delta, z * rows, rows, 0)
    own_up = lax.dynamic_slice_in_dim(up_delta, z * rows, rows, 0)
    terms = contract_cols(own_gate, w_gate) + contract_cols(own_up, w_upward)
    grad_input = plane_sum(chips, across, terms.astype(jnp.bfloat16))

    cols = width // reps
    input_cols = lax.dynamic_slice_in_dim(all_inputs, z * cols, cols, 1)
    cotangent_cols = lax.dynamic_slice_in_dim(all_cotangent, z * cols, cols, 1)
    grad_gate = contract_rows(input_cols, gate_delta)
    grad_upward = contract_rows(input_cols, up_delta)
    grad_down = contract_rows(hidden, cotangent_cols)
    return (grad_input, grad_gate, grad_upward, grad_down)


def solution(mesh):
    across = mesh.shape["tp"] // 2
    chips = mesh.shape["fs"] * across
    in_specs = (
        P("rep", None),
        P("rep", None),
        P(None, PLANE),
        P(None, PLANE),
        P(PLANE, None),
    )
    out_specs = (
        P("rep", None),
        P("rep", PLANE),
        P("rep", PLANE),
        P(PLANE, "rep"),
    )
    body = functools.partial(local, mesh.shape["rep"], chips, across)
    return jax.shard_map(body, mesh=mesh, in_specs=in_specs, out_specs=out_specs, check_vma=False)
```

```python
import functools

import jax
import jax.numpy as jnp
from jax import lax
from jax.experimental import pallas as pl
from jax.experimental.pallas import tpu as pltpu
from jax.sharding import PartitionSpec as P

PLANE = ("fs", "tp")
MESH = pl.DeviceIdType.MESH
STREAM = (256, 256, 512, 384)
BLOCK = (512, 512, 384)
FLIGHT = 4


def contract_rows(left, right):
    return lax.dot_general(
        left, right, (((0,), (0,)), ((), ())), preferred_element_type=jnp.float32
    )


def contract_cols(left, right):
    return lax.dot_general(
        left, right, (((1,), (1,)), ((), ())), preferred_element_type=jnp.float32
    )


def greet(neighbours):
    barrier = pltpu.get_barrier_semaphore()
    for device in neighbours:
        pl.semaphore_signal(barrier, inc=1, device_id=device, device_id_type=MESH)
    pl.semaphore_wait(barrier, len(neighbours))


def gather_kernel(reps, x_ref, c_ref, all_x, all_c, send, recv, own_sem):
    z, y, t = lax.axis_index("rep"), lax.axis_index("fs"), lax.axis_index("tp")
    x, core = t // 2, t % 2
    half = (x + y) % 2
    mine = 2 * half + core
    across = 2 * (1 - half) + core
    up, down = (z + 1) % reps, (z + reps - 1) % reps
    to_up, to_down = (up, y, t), (down, y, t)
    x_near = (z, y, 2 * (x + 1 - 2 * (x % 2)) + core)
    y_near = (z, y + 1 - 2 * (y % 2), t)
    other = (z, y, 2 * x + 1 - core)
    greet((to_up, to_down, x_near, y_near, other))

    started = []

    def put(kind, step, src, dst, device):
        copy = pltpu.make_async_remote_copy(
            src_ref=src, dst_ref=dst, send_sem=send.at[kind, step],
            recv_sem=recv.at[kind, step], device_id=device, device_id_type=MESH,
        )
        copy.start()
        started.append(copy)
        return copy

    ring = [
        put(0, 0, x_ref.at[mine], all_x.at[z, mine], to_up),
        put(1, 0, c_ref.at[mine], all_c.at[z, mine], to_down),
    ]
    keep = [
        pltpu.make_async_copy(x_ref, all_x.at[z], own_sem.at[0]),
        pltpu.make_async_copy(c_ref, all_c.at[z], own_sem.at[1]),
    ]
    for copy in keep:
        copy.start()

    last = []

    def relay(sides, step, bx, bc):
        sides[0].wait_recv()
        last.append(put(6, step, all_x.at[bx, across], all_x.at[bx, across], other))
        sides[1].wait_recv()
        last.append(put(7, step, all_c.at[bc, across], all_c.at[bc, across], other))

    before = None
    for step in range(reps - 1):
        bx, bc = (z + reps - 1 - step) % reps, (z + 1 + step) % reps
        got_x, got_c = all_x.at[bx, mine], all_c.at[bc, mine]
        following = []
        ring[0].wait_recv()
        if step < reps - 2:
            following.append(put(0, step + 1, got_x, got_x, to_up))
        side_x = put(2, step, got_x, got_x, x_near)
        last.append(put(4, step, got_x, got_x, other))
        ring[1].wait_recv()
        if step < reps - 2:
            following.append(put(1, step + 1, got_c, got_c, to_down))
        side_c = put(3, step, got_c, got_c, y_near)
        last.append(put(5, step, got_c, got_c, other))
        if before is not None:
            relay(*before)
        before = ((side_x, side_c), step, bx, bc)
        ring = following
    relay(*before)
    for copy in last:
        copy.wait_recv()
    for copy in started:
        copy.wait_send()
    for copy in keep:
        copy.wait()


def gather(reps, inputs, cotangent):
    rows, width = inputs.shape
    quarter = (4, rows // 4, width)
    whole = jax.ShapeDtypeStruct((reps,) + quarter, inputs.dtype)
    vmem = pl.BlockSpec(memory_space=pltpu.VMEM)
    pair = pl.pallas_call(
        functools.partial(gather_kernel, reps),
        out_shape=(whole, whole),
        in_specs=[vmem, vmem],
        out_specs=(vmem, vmem),
        scratch_shapes=[
            pltpu.SemaphoreType.DMA((8, reps - 1)),
            pltpu.SemaphoreType.DMA((8, reps - 1)),
            pltpu.SemaphoreType.DMA((2,)),
        ],
        compiler_params=pltpu.CompilerParams(
            collective_id=0, has_side_effects=True, vmem_limit_bytes=60 * 2**20
        ),
        name="token_gather",
    )(inputs.reshape(quarter), cotangent.reshape(quarter))
    return [a.reshape(reps * rows, width) for a in pair]


def reduce_kernel(chips, across, terms, out, got, sums, landed, send, recv):
    z, y, t = lax.axis_index("rep"), lax.axis_index("fs"), lax.axis_index("tp")
    core = t % 2
    chip = y * across + t // 2
    other = (z, y, t + 1 - 2 * core)

    def peer(ahead):
        there = (chip + ahead) % chips
        return there, (z, there // across, 2 * (there % across) + core)

    greet([other] + [peer(ahead)[1] for ahead in range(1, chips)])

    def put(kind, slot, src, dst, device):
        copy = pltpu.make_async_remote_copy(
            src_ref=src, dst_ref=dst, send_sem=send.at[kind, slot],
            recv_sem=recv.at[kind, slot], device_id=device, device_id_type=MESH,
        )
        copy.start()
        return copy

    swaps = [put(0, j, terms.at[j, 1 - core], got.at[j], other) for j in range(chips)]
    for j in range(chips):
        swaps[j].wait_recv()
        pair = terms[j, core].astype(jnp.float32) + got[j].astype(jnp.float32)
        sums[j] = pair.astype(sums.dtype)
    spread = []
    for ahead in range(1, chips):
        there, device = peer(ahead)
        spread.append(put(1, ahead, sums.at[there], landed.at[ahead], device))
    total = terms[chip, core].astype(jnp.float32) + got[chip].astype(jnp.float32)
    for ahead in range(1, chips):
        spread[ahead - 1].wait_recv()
        total = total + landed[ahead].astype(jnp.float32)
    out[chip, core] = total.astype(out.dtype)
    done = out.at[chip, core]
    share = [put(2, ahead, done, done, peer(ahead)[1]) for ahead in range(1, chips)]
    relays = [put(3, 0, done, done, other)]
    for ahead in range(1, chips):
        share[ahead - 1].wait_recv()
        source = out.at[(chip + chips - ahead) % chips, core]
        relays.append(put(3, ahead, source, source, other))
    for copy in relays:
        copy.wait_recv()
    for copy in swaps + spread + share + relays:
        copy.wait_send()


def plane_sum(chips, across, terms):
    rows, width = terms.shape
    piece = (rows // (2 * chips), width)
    vmem = pl.BlockSpec(memory_space=pltpu.VMEM)
    total = pl.pallas_call(
        functools.partial(reduce_kernel, chips, across),
        out_shape=jax.ShapeDtypeStruct((chips, 2) + piece, terms.dtype),
        in_specs=[vmem],
        out_specs=vmem,
        scratch_shapes=[
            pltpu.VMEM((chips,) + piece, terms.dtype),
            pltpu.VMEM((chips,) + piece, terms.dtype),
            pltpu.VMEM((chips,) + piece, terms.dtype),
            pltpu.SemaphoreType.DMA((4, chips)),
            pltpu.SemaphoreType.DMA((4, chips)),
        ],
        compiler_params=pltpu.CompilerParams(
            collective_id=1, has_side_effects=True, vmem_limit_bytes=48 * 2**20
        ),
        name="plane_sum",
    )(terms.reshape((chips, 2) + piece))
    return total.reshape(rows, width)


def chunks_of(total, widths):
    spans, at = [], 0
    for width in widths:
        if at < total:
            spans.append((at, min(width, total - at)))
            at += width
    while at < total:
        spans.append((at, min(widths[-1], total - at)))
        at += widths[-1]
    return spans


def fused_kernel(
    reps, chips, across, x_hbm, c_hbm, wg_hbm, wu_hbm, wd_hbm,
    out, hid, gd, ud, xc, cc,
    all_x, all_c, wg, wu, wd, gpre, upre, got, landed,
    send, recv, sum_send, sum_recv, local_sem, weight_sem,
):
    z, y, t = lax.axis_index("rep"), lax.axis_index("fs"), lax.axis_index("tp")
    x, core = t // 2, t % 2
    rows, width = all_x.shape[1:]
    hidden = wg.shape[1]
    cols = width // reps
    chip = y * across + x
    x_chip, y_chip = y * across + 1 - x, (1 - y) * across + x
    far_chip = (1 - y) * across + 1 - x
    x_near, y_near = (z, y, 2 * (1 - x) + core), (z, 1 - y, t)
    other = (z, y, 2 * x + 1 - core)
    near = (z, jnp.where(core == 0, y, 1 - y), jnp.where(core == 0, 2 * (1 - x) + core, t))
    crosswise = (z, jnp.where(core == 0, 1 - y, y), jnp.where(core == 0, t, 2 * (1 - x) + core))
    half = (x + y) % 2

    def peer(ahead):
        there = (chip + ahead) % chips
        return there, (z, there // across, 2 * (there % across) + core)

    def part_of(parts, index):
        size = rows // parts
        return pl.ds(pl.multiple_of(index * size, size), size)

    def x_part(of_chip, of_core):
        return part_of(8, 2 * of_chip + of_core)

    def c_part(of_half, of_core):
        return part_of(4, 2 * of_half + of_core)

    local = [
        pltpu.make_async_copy(x_hbm, all_x.at[0], local_sem.at[0]),
        pltpu.make_async_copy(c_hbm, all_c.at[0], local_sem.at[1]),
    ]
    for copy in local:
        copy.start()
    stream = chunks_of(hidden, STREAM)
    weights = []
    for n, (at, size) in enumerate(stream):
        span = pl.ds(at, size)
        weights += [
            pltpu.make_async_copy(wg_hbm.at[:, span], wg.at[:, span], weight_sem.at[n, 0]),
            pltpu.make_async_copy(wu_hbm.at[:, span], wu.at[:, span], weight_sem.at[n, 1]),
            pltpu.make_async_copy(wd_hbm.at[span], wd.at[span], weight_sem.at[n, 2]),
        ]
    for copy in weights[:FLIGHT]:
        copy.start()

    def weight_ready(n):
        weights[n].wait()
        if n + FLIGHT < len(weights):
            weights[n + FLIGHT].start()

    greet(
        [((z + 1) % reps, y, t), ((z + reps - 1) % reps, y, t), other]
        + [peer(ahead)[1] for ahead in range(1, chips)]
    )

    def slot_of(level, block):
        step = jnp.where(block < level, level - block, block - level) - 1
        fewer = jnp.minimum(level, reps - 1 - level)
        paired = 2 * step + jnp.where(block < level, 0, 1)
        return 1 + jnp.where(step < fewer, paired, step + fewer)

    def make(kind, slot, src, dst, device, sender=None, there=None):
        return pltpu.make_async_remote_copy(
            src_ref=src, dst_ref=dst, send_sem=send.at[kind if sender is None else sender, slot],
            recv_sem=recv.at[kind, slot if there is None else there],
            device_id=device, device_id_type=MESH,
        )

    def pass_on(buffer, kind, slot, part, device):
        piece = buffer.at[slot, part]
        return make(kind, slot, piece, piece, device)

    def hop_on(buffer, kind, slot, part, device, there):
        return make(kind, slot, buffer.at[slot, part], buffer.at[there, part], device, None, there)

    above, below = jnp.minimum(z + 1, reps - 1), jnp.maximum(z - 1, 0)
    up, down = (above, y, t), (below, y, t)

    def first_sends():
        sends = []
        for kind, src, buffer, part in (
            (0, x_hbm, all_x, x_part(chip, core)), (8, c_hbm, all_c, c_part(half, core))
        ):
            for wanted, device, level, sender in (
                (z < reps - 1, up, above, kind), (z > 0, down, below, 12 + kind // 8)
            ):
                there = slot_of(level, z)
                copy = make(kind, 0, src.at[part], buffer.at[there, part], device, sender, there)
                sends.append((wanted, copy))
        return sends

    def sides(step):
        low, high = z - 1 - step, z + 1 + step
        from_low, from_high = jnp.maximum(low, 0), jnp.minimum(high, reps - 1)
        return (
            (low >= 0, slot_of(z, from_low), up, slot_of(above, from_low), (low >= 0) & (z < reps - 1)),
            (high < reps, slot_of(z, from_high), down, slot_of(below, from_high), (high < reps) & (z > 0)),
        )

    def hops(buffer, kind, part, step):
        for valid, slot, onward, there, passes in sides(step):
            yield valid, pass_on(buffer, kind, slot, part, other), passes, hop_on(buffer, kind, slot, part, onward, there)

    def hop(array, step):
        buffer, kind, part = ((all_x, 0, x_part(chip, core)), (all_c, 8, c_part(half, core)))[array]
        for valid, arrived, passes, onward in hops(buffer, kind, part, step):
            pl.when(valid)(arrived.wait_recv)
            pl.when(passes)(onward.start)

    beside, across_y, opposite = x_part(x_chip, core), x_part(y_chip, core), x_part(far_chip, core)
    turned = part_of(8, 2 * jnp.where(core == 0, x_chip, y_chip) + core)

    def near_x(slot):
        part = x_part(chip, core)
        return [
            pass_on(all_x, 1, slot, part, x_near), pass_on(all_x, 2, slot, part, y_near),
            pass_on(all_x, 4, slot, part, other),
        ]

    def spread_x(slot):
        return [
            pass_on(all_x, 3, slot, turned, crosswise), pass_on(all_x, 5, slot, beside, other),
            pass_on(all_x, 6, slot, across_y, other),
        ]

    def last_x(slot):
        return [pass_on(all_x, 7, slot, opposite, other)]

    def near_c(slot):
        part = c_part(half, core)
        return [pass_on(all_c, 9, slot, part, near), pass_on(all_c, 10, slot, part, other)]

    def last_c(slot):
        return [pass_on(all_c, 11, slot, c_part(1 - half, core), other)]

    awaited = {
        near_x: (), near_c: (), spread_x: ((1, beside), (2, across_y)), last_x: ((3, opposite),),
        last_c: ((9, c_part(1 - half, core)),),
    }

    def serve(service, slot):
        buffer = all_c if service in (near_c, last_c) else all_x
        for kind, part in awaited[service]:
            pass_on(buffer, kind, slot, part, other).wait_recv()
        for copy in service(slot):
            copy.start()

    def complete_x(slot):
        for kind in range(4, 8):
            pass_on(all_x, kind, slot, x_part(chip, core), other).wait_recv()
        keep_cols(all_x, xc, slot)

    def complete_c(slot):
        for kind in range(10, 12):
            pass_on(all_c, kind, slot, c_part(half, core), other).wait_recv()
        keep_cols(all_c, cc, slot)

    def pre(slot, place, at, size):
        span, held = pl.ds(at, size), pl.ds(place * rows, rows)
        tokens = all_x[slot]
        gpre[held, span] = jnp.dot(tokens, wg[:, span], preferred_element_type=jnp.float32)
        upre[held, span] = jnp.dot(tokens, wu[:, span], preferred_element_type=jnp.float32)

    def deltas(slot, count, at, size):
        span, held, slots = pl.ds(at, size), pl.ds(0, count * rows), pl.ds(slot, count)
        tokens = all_c[slots].reshape(count * rows, width)
        grad = contract_cols(tokens, wd[span, :])
        gate, lift = gpre[held, span], upre[held, span]
        sig = jax.nn.sigmoid(gate)
        act = gate * sig
        shape = (count, rows, size)
        hid[slots, :, span] = (act * lift).astype(hid.dtype).reshape(shape)
        gate_grad = grad * lift * sig * (1.0 + gate * (1.0 - sig))
        gd[slots, :, span] = gate_grad.astype(gd.dtype).reshape(shape)
        ud[slots, :, span] = (grad * act).astype(ud.dtype).reshape(shape)

    def keep_cols(buffer, kept, slot):
        span = pl.ds(pl.multiple_of(z * cols, cols), cols)
        kept[slot] = buffer[slot, :, span]

    small = rows // (2 * chips)

    def term(piece, of_core):
        return all_c.at[0, part_of(2 * chips, 2 * piece + of_core)]

    def pair_sum(ahead):
        return all_x.at[0, pl.ds((ahead - 1) * small, small)]

    def sum_copy(kind, slot, src, dst, device):
        return pltpu.make_async_remote_copy(
            src_ref=src, dst_ref=dst, send_sem=sum_send.at[kind, slot],
            recv_sem=sum_recv.at[kind, slot], device_id=device, device_id_type=MESH,
        )

    def swaps():
        return [sum_copy(0, j, term(j, 1 - core), got.at[j], other) for j in range(chips)]

    def spread():
        return [
            sum_copy(1, ahead, pair_sum(ahead), landed.at[ahead - 1], peer(ahead)[1])
            for ahead in range(1, chips)
        ]

    def share():
        done = out.at[chip, core]
        return [sum_copy(2, ahead, done, done, peer(ahead)[1]) for ahead in range(1, chips)]

    def relays():
        sources = [out.at[(chip + chips - ahead) % chips, core] for ahead in range(chips)]
        return [sum_copy(3, ahead, source, source, other) for ahead, source in enumerate(sources)]

    def reduce_first():
        for copy in swaps():
            copy.wait_recv()
        for ahead in range(1, chips):
            there = peer(ahead)[0]
            pair = term(there, core)[...].astype(jnp.float32) + got[there].astype(jnp.float32)
            pair_sum(ahead)[...] = pair.astype(got.dtype)
        for copy in spread():
            copy.start()

    def reduce_second():
        total = term(chip, core)[...].astype(jnp.float32) + got[chip].astype(jnp.float32)
        for ahead, copy in enumerate(spread()):
            copy.wait_recv()
            total = total + landed[ahead].astype(jnp.float32)
        out[chip, core] = total.astype(out.dtype)
        for copy in share():
            copy.start()
        relays()[0].start()

    def reduce_third():
        for copy, onward in zip(share(), relays()[1:]):
            copy.wait_recv()
            onward.start()

    for condition, copy in first_sends():
        pl.when(condition)(copy.start)
    for copy in local:
        copy.wait()
    keep_cols(all_x, xc, 0)
    keep_cols(all_c, cc, 0)
    slots = {
        (0, 1): ((hop, 0, 0), (serve, near_x, 1)),
        (1, 2): ((serve, spread_x, 1), (hop, 1, 0), (serve, near_c, 1)),
        (1, 3): ((hop, 0, 1), (serve, near_x, 2)),
        (2, 0): ((serve, last_x, 1),),
        (2, 2): ((serve, last_c, 1), (hop, 1, 1), (serve, near_c, 2)),
        (2, 3): ((serve, spread_x, 2),),
        (3, 0): ((hop, 0, 2), (serve, near_x, 3)),
        (3, 2): ((serve, last_x, 2),),
        (4, 0): ((serve, last_c, 2),),
        (4, 1): ((serve, spread_x, 3),),
        (4, 2): ((hop, 1, 2), (serve, near_c, 3)),
        (5, 2): ((serve, last_x, 3), (reduce_second,)),
        (6, 1): ((serve, last_c, 3),),
        (7, 1): ((reduce_third,),),
    }

    def at_slot(phase, n):
        for action, *details in slots.get((phase, n), ()):
            action(*details)

    for n, (at, size) in enumerate(stream):
        weight_ready(3 * n)
        weight_ready(3 * n + 1)
        pre(0, 0, at, size)
        at_slot(0, n)
        weight_ready(3 * n + 2)
        deltas(0, 1, at, size)
        at_slot(1, n)

    part = width // 4
    for n in range(4):
        span = pl.ds(n * part, part)
        total = contract_cols(gd[0], wg[span, :]) + contract_cols(ud[0], wu[span, :])
        all_c[0, :, span] = total.astype(all_c.dtype)
        at_slot(2, n)
    for copy in swaps():
        copy.start()

    blocks = chunks_of(hidden, BLOCK)
    complete_x(1)
    for n, (at, size) in enumerate(blocks):
        pre(1, 0, at, size)
        at_slot(3, n)
        if n == 1:
            reduce_first()
    complete_c(1)
    for n, (at, size) in enumerate(blocks):
        deltas(1, 1, at, size)
        at_slot(4, n)
    complete_x(2)
    for n, (at, size) in enumerate(blocks):
        pre(2, 0, at, size)
        at_slot(5, n)
    complete_x(3)
    for n, (at, size) in enumerate(blocks):
        pre(3, 1, at, size)
        at_slot(6, n)
    complete_c(2)
    complete_c(3)
    for n, (at, size) in enumerate(blocks):
        deltas(2, 2, at, size)
        at_slot(7, n)
    for copy in relays():
        copy.wait_recv()
    for condition, copy in first_sends():
        pl.when(condition)(copy.wait_send)
    for copy in swaps() + spread() + share() + relays():
        copy.wait_send()

    for slot in range(1, reps):
        for service in (near_x, spread_x, last_x, near_c, last_c):
            for copy in service(slot):
                copy.wait_send()
    for step in range(reps - 1):
        for buffer, kind, part in ((all_x, 0, x_part(chip, core)), (all_c, 8, c_part(half, core))):
            for _, _, passes, onward in hops(buffer, kind, part, step):
                pl.when(passes)(onward.wait_send)


def fused(reps, chips, across, inputs, cotangent, w_gate, w_upward, w_down):
    rows, width = inputs.shape
    hidden = w_gate.shape[1]
    cols = width // reps
    kind = inputs.dtype
    piece = (rows // (2 * chips), width)
    vmem = pl.BlockSpec(memory_space=pltpu.VMEM)
    anywhere = pl.BlockSpec(memory_space=pl.ANY)
    count = len(chunks_of(hidden, STREAM))
    wide = jax.ShapeDtypeStruct((reps, rows, hidden), kind)
    slim = jax.ShapeDtypeStruct((reps, rows, cols), kind)
    total, hid, gd, ud, xc, cc = pl.pallas_call(
        functools.partial(fused_kernel, reps, chips, across),
        out_shape=(jax.ShapeDtypeStruct((chips, 2) + piece, kind), wide, wide, wide, slim, slim),
        in_specs=[pl.BlockSpec(memory_space=pltpu.HBM)] * 5,
        out_specs=(vmem,) * 6,
        scratch_shapes=[
            pltpu.VMEM((reps, rows, width), kind),
            pltpu.VMEM((reps, rows, width), kind),
            pltpu.VMEM((width, hidden), kind),
            pltpu.VMEM((width, hidden), kind),
            pltpu.VMEM((hidden, width), kind),
            pltpu.VMEM((2 * rows, hidden), jnp.float32),
            pltpu.VMEM((2 * rows, hidden), jnp.float32),
            pltpu.VMEM((chips,) + piece, kind),
            pltpu.VMEM((chips - 1,) + piece, kind),
            pltpu.SemaphoreType.DMA((14, reps)),
            pltpu.SemaphoreType.DMA((12, reps)),
            pltpu.SemaphoreType.DMA((4, chips)),
            pltpu.SemaphoreType.DMA((4, chips)),
            pltpu.SemaphoreType.DMA((2,)),
            pltpu.SemaphoreType.DMA((count, 3)),
        ],
        compiler_params=pltpu.CompilerParams(
            collective_id=2, has_side_effects=True, vmem_limit_bytes=46 * 2**20 + 704 * 2**10
        ),
        name="gather_compute",
    )(*(pltpu.with_memory_space_constraint(a, pltpu.HBM) for a in (inputs, cotangent, w_gate, w_upward, w_down)))
    return total.reshape(rows, width), [a.reshape(reps * rows, -1) for a in (hid, gd, ud, xc, cc)]


def weights_kernel(tall, wide_rows, hid, gd, ud, xc, cc, total, g_gate, g_up, g_down, g_in, stage, stage_down, sems, down_sems, in_sem):
    whole = pltpu.make_async_copy(total, g_in, in_sem)
    whole.start()
    pending = [None] * stage.shape[0]
    turn = 0
    for at, size in chunks_of(xc.shape[1], (tall,)):
        turned = xc[:, pl.ds(at, size)].T
        for delta, target in ((gd, g_gate), (ud, g_up)):
            slot = turn % len(pending)
            if pending[slot] is not None:
                pending[slot].wait()
            span = pl.ds(at, size)
            stage[slot, :size] = jnp.dot(turned, delta[...], preferred_element_type=jnp.float32)
            pending[slot] = pltpu.make_async_copy(stage.at[slot, pl.ds(0, size)], target.at[span], sems.at[slot])
            pending[slot].start()
            turn += 1
    later = [None] * stage_down.shape[0]
    turn = 0
    for at, size in chunks_of(hid.shape[1], (wide_rows,)):
        slot = turn % len(later)
        if later[slot] is not None:
            later[slot].wait()
        span = pl.ds(at, size)
        stage_down[slot, :size] = contract_rows(hid[:, span], cc[...])
        later[slot] = pltpu.make_async_copy(stage_down.at[slot, pl.ds(0, size)], g_down.at[span], down_sems.at[slot])
        later[slot].start()
        turn += 1
    for copy in pending + later:
        if copy is not None:
            copy.wait()
    whole.wait()


def weight_gradients(total, hid, gd, ud, xc, cc):
    hidden, cols = hid.shape[1], xc.shape[1]
    vmem = pl.BlockSpec(memory_space=pltpu.VMEM)
    anywhere = pl.BlockSpec(memory_space=pl.ANY)
    up = jax.ShapeDtypeStruct((cols, hidden), jnp.float32)
    down = jax.ShapeDtypeStruct((hidden, cols), jnp.float32)
    tall, wide_rows, slots = 256, 384, 3
    return pl.pallas_call(
        functools.partial(weights_kernel, tall, wide_rows),
        out_shape=(up, up, down, jax.ShapeDtypeStruct(total.shape, total.dtype)),
        in_specs=[vmem] * 6,
        out_specs=(anywhere,) * 4,
        scratch_shapes=[
            pltpu.VMEM((slots, tall, hidden), jnp.float32),
            pltpu.VMEM((slots, wide_rows, cols), jnp.float32),
            pltpu.SemaphoreType.DMA((slots,)),
            pltpu.SemaphoreType.DMA((slots,)),
            pltpu.SemaphoreType.DMA,
        ],
        compiler_params=pltpu.CompilerParams(vmem_limit_bytes=20 * 2**20),
        name="weight_gradients",
    )(hid, gd, ud, xc, cc, total)


def fits(reps, chips, across, inputs, w_gate):
    rows, width = inputs.shape
    hidden = w_gate.shape[1]
    size = inputs.dtype.itemsize
    need = size * (3 * width * hidden + 2 * reps * rows * width + 3 * reps * rows * hidden)
    aligned = hidden % 128 == 0 and width % (128 * reps) == 0 and rows % 128 == 0
    return aligned and chips == 4 and across == 2 and reps == 4 and need < 52 * 2**20


def local(reps, chips, across, inputs, cotangent, w_gate, w_upward, w_down):
    rows, width = inputs.shape
    if fits(reps, chips, across, inputs, w_gate):
        total, parts = fused(reps, chips, across, inputs, cotangent, w_gate, w_upward, w_down)
        grad_gate, grad_upward, grad_down, grad_input = weight_gradients(total, *parts)
        return (grad_input, grad_gate, grad_upward, grad_down)
    all_inputs, all_cotangent = gather(reps, inputs, cotangent)

    gate_pre = jnp.dot(all_inputs, w_gate, preferred_element_type=jnp.float32)
    up_pre = jnp.dot(all_inputs, w_upward, preferred_element_type=jnp.float32)
    sigmoid_gate = jax.nn.sigmoid(gate_pre)
    activated = gate_pre * sigmoid_gate
    hidden = (activated * up_pre).astype(jnp.bfloat16)
    hidden_grad = contract_cols(all_cotangent, w_down)
    gate_delta = (
        hidden_grad * up_pre * sigmoid_gate * (1.0 + gate_pre * (1.0 - sigmoid_gate))
    ).astype(jnp.bfloat16)
    up_delta = (hidden_grad * activated).astype(jnp.bfloat16)

    z = lax.axis_index("rep")
    own_gate = lax.dynamic_slice_in_dim(gate_delta, z * rows, rows, 0)
    own_up = lax.dynamic_slice_in_dim(up_delta, z * rows, rows, 0)
    terms = contract_cols(own_gate, w_gate) + contract_cols(own_up, w_upward)
    grad_input = plane_sum(chips, across, terms.astype(jnp.bfloat16))

    cols = width // reps
    input_cols = lax.dynamic_slice_in_dim(all_inputs, z * cols, cols, 1)
    cotangent_cols = lax.dynamic_slice_in_dim(all_cotangent, z * cols, cols, 1)
    grad_gate = contract_rows(input_cols, gate_delta)
    grad_upward = contract_rows(input_cols, up_delta)
    grad_down = contract_rows(hidden, cotangent_cols)
    return (grad_input, grad_gate, grad_upward, grad_down)


def solution(mesh):
    across = mesh.shape["tp"] // 2
    chips = mesh.shape["fs"] * across
    in_specs = (
        P("rep", None),
        P("rep", None),
        P(None, PLANE),
        P(None, PLANE),
        P(PLANE, None),
    )
    out_specs = (
        P("rep", None),
        P("rep", PLANE),
        P("rep", PLANE),
        P(PLANE, "rep"),
    )
    body = functools.partial(local, mesh.shape["rep"], chips, across)
    return jax.shard_map(body, mesh=mesh, in_specs=in_specs, out_specs=out_specs, check_vma=False)
```
